256 devices in a mesh: ep: 64 (over z, y, core), tp: 4 (over x).
Axes of the slice: x: 4, y: 4, z: 8, core: 2. Of those that a mesh axis runs over, the one named last changes fastest.
Arguments:
- query_latent: bfloat16 [8192, 768], P('ep'), may hold values from -6 to 6
- keyval_latent: bfloat16 [8192, 512], P('ep'), may hold values from -6 to 6
- rotary_key: bfloat16 [8192, 32], P('ep'), may hold values from -6 to 6
- query_gain: float32 [768], replicated, may hold values from 0.3 to 48
- keyval_gain: float32 [512], replicated, may hold values from 0.1 to 1.9
- query_weight: bfloat16 [768, 1536], P(None, 'tp'), may hold values from -0.21875 to 0.21875
- keyval_weight: bfloat16 [512, 2048], P(None, 'tp'), may hold values from -0.25 to 0.25
- output_weight: bfloat16 [1024, 2048], P('tp'), may hold values from -0.1875 to 0.1875
- output_gain: float32 [2048], replicated, may hold values from 0.1 to 1.9
- second_rows: bfloat16 [8192, 2048], P('ep'), may hold values from -6 to 6
- second_gain: float32 [2048], replicated, may hold values from 0.1 to 1.9
- route_ids: int32 [8192, 4], P('ep'), may hold values from 0 to 63, all different within a row; in each aligned block of 128 rows (0 to 127, 128 to 255, ...) at most 16 rows name the same one
- route_weights: float32 [8192, 4], P('ep'), may hold values from 0.1 to 1
- gate_weight: bfloat16 [64, 2048, 1024], P('ep', None, 'tp'), may hold values from -0.125 to 0.125
- up_weight: bfloat16 [64, 2048, 1024], P('ep', None, 'tp'), may hold values from -0.125 to 0.125
- down_weight: bfloat16 [64, 1024, 2048], P('ep', 'tp'), may hold values from -0.1875 to 0.1875
- shared_gate: bfloat16 [2048, 512], P(None, 'tp'), may hold values from -0.125 to 0.125
- shared_up: bfloat16 [2048, 512], P(None, 'tp'), may hold values from -0.125 to 0.125
- shared_down: bfloat16 [512, 2048], P('tp'), may hold values from -0.25 to 0.25
Outputs:
- mixed: bfloat16 [8192, 2048], P(('ep', 'tp'))
- expert_mix: bfloat16 [8192, 2048], P('ep', 'tp')
The draws below stay inside these ranges and needn't reach their ends.
Inputs may be any that keep to these rules, and one draw needn't show every extreme that they name: `route_ids`: each row names 4 different experts. Among the rows of one index of ep (aligned blocks of 128 rows) no expert is named more than 16 times, a bound that some expert reaches in some blocks.
All inputs are finite; a program needn't handle non-finite values.
Results may differ from the reference program's by a relative error of at most 0.023.
The reference program's roundings to bfloat16 on the way count: a program that leaves them out, or rounds other values in their place, can miss the bound.
Values may be sent and summed in bfloat16 or wider, within the bound.
A program may use at most 128 MiB of HBM per device.

```python
import math
import jax
import jax.numpy as jnp
import numpy as np
from jax import lax

D = 2048
HEADS = 16
NOPE = 64
ROPE = 32
VDIM = 64
QLAT = 768
KVLAT = 512
FE = 1024
FS = 512
TOP = 4
TOKB = 128
SEQ = 8192
TOKENS_B = 8192
EXPERTS = 64
CAP = 16
N_EP = 64
N_TP = 4


def draw_query_gain(key, part):
    return jax.random.uniform(key, (QLAT,), jnp.float32, 0.3, 1.7)


def levels(key, extent, cuts, low, largest):
    def one(axis_at, blocks):
        draws = jax.random.uniform(jax.random.fold_in(jax.random.fold_in(key, 6), axis_at), (blocks,), jnp.float32, low / len(cuts), largest / len(cuts))
        return jnp.repeat(jnp.exp(draws), extent[axis_at] // blocks).reshape((-1,) + (1,) * (len(extent) - axis_at - 1))

    loudness = one(*cuts[0])
    for cut in cuts[1:]:
        loudness = loudness * one(*cut)
    return loudness


def assign_block(stream_key, own, number, rows, count, top, bound, lean):
    ranking = jax.random.permutation(stream_key, count)
    packed, common = shares(count, rows * top, bound, lean, True), shares(count, rows * top, bound, lean, False)
    places = jnp.arange(count)

    def named(tallies, turn):
        used = int((tallies > 0).sum())
        fixed = max(1, used // 4)
        moved = fixed + (places - fixed + turn * (used - fixed)) % max(1, count - fixed)
        return jnp.zeros((count,), jnp.int32).at[ranking[jnp.where(places < fixed, places, moved)]].set(jnp.asarray(tallies, jnp.int32))

    tallies = jnp.where(number % 4 == 0, named(packed, number // 4), named(common, number - number // 4 - 1))
    mixed = jax.random.permutation(jax.random.fold_in(own, 3), count)
    source_of, taker = mixed[0:count // 2 * 2:2], mixed[1:count // 2 * 2:2]
    margin = jnp.minimum(tallies[source_of] - 1, bound - tallies[taker]) // 2
    margin = jnp.where((source_of == ranking[0]) | (taker == ranking[0]) | (tallies[taker] == 0), 0, jnp.maximum(margin, 0))
    moved = jax.random.randint(jax.random.fold_in(own, 4), (count // 2,), 0, 1 << 20) % (margin + 1)
    tallies = tallies.at[source_of].add(-moved).at[taker].add(moved)
    labels = jnp.searchsorted(jnp.cumsum(tallies), jnp.arange(rows * top), side="right").astype(jnp.int32)
    table = labels.reshape(top, rows).T
    table = table[jax.random.permutation(jax.random.fold_in(own, 1), rows)]
    turn = jax.random.randint(jax.random.fold_in(own, 2), (rows, 1), 0, top)
    return jnp.take_along_axis(table, (jnp.arange(top)[None, :] + turn) % top, axis=1)


def shares(amount, total, reach, skew, full):
    portions = [(1 << 20) // math.isqrt(grade ** skew) + 1 for grade in range(1, amount + 1)]
    largest = reach if full else min(reach, max(-(-total // amount), total * portions[0] // sum(portions)))
    least = 1 if total - largest >= amount - 1 else 0
    holding, spare = [largest] + [least] * (amount - 1), total - largest - least * (amount - 1)
    while spare > 0:
        movable = [i for i in range(1, amount) if holding[i] < largest] or [i for i in range(1, amount) if holding[i] < reach]
        mass, left = sum([portions[i] for i in movable]), spare
        for i in movable:
            more = min(reach - holding[i], max(1, left * portions[i] // mass), spare)
            holding[i] = holding[i] + more
            spare = spare - more
    return np.array(holding)


def scatter_about(own_key, dims, spread, limit, shards=(), held_as=jnp.bfloat16):
    values = spread * jax.random.normal(own_key, dims, jnp.float32)
    if shards:
        values = values * levels(own_key, dims, shards, -0.22, 0.18)
    return jnp.clip(values, -limit, limit).astype(held_as)


def setup_inputs(seed: int = 0) -> dict:
    seeds = jax.random.split(jax.random.key(seed), 20)
    query_latent = scatter_about(seeds[0], (SEQ, QLAT), 1.0, 6.0, ((0, 64),))
    keyval_latent = scatter_about(seeds[1], (SEQ, KVLAT), 1.0, 6.0, ((0, 64),))
    rotary_key = scatter_about(seeds[2], (SEQ, ROPE), 1.0, 6.0, ((0, 64),))
    query_gain = draw_query_gain(jax.random.fold_in(seeds[19], 71), 0)
    keyval_gain = jnp.clip(1.0 + 0.18 * jax.random.normal(seeds[4], (KVLAT,), jnp.float32), 0.1, 1.9)
    query_weight = scatter_about(seeds[5], (QLAT, HEADS * (NOPE + ROPE)), QLAT ** -0.5, 0.21875, ((1, 4),))
    keyval_weight = scatter_about(seeds[6], (KVLAT, HEADS * (NOPE + VDIM)), KVLAT ** -0.5, 0.25, ((1, 4),))
    output_weight = scatter_about(seeds[7], (HEADS * VDIM, D), (HEADS * VDIM) ** -0.5, 0.1875, ((0, 4),))
    output_gain = jnp.clip(1.0 + 0.18 * jax.random.normal(seeds[8], (D,), jnp.float32), 0.1, 1.9)
    second_rows = scatter_about(seeds[9], (TOKENS_B, D), 1.0, 6.0, ((0, 64),))
    second_gain = jnp.clip(1.0 + 0.18 * jax.random.normal(seeds[10], (D,), jnp.float32), 0.1, 1.9)
    route_ids_keys = jax.random.split(jax.random.fold_in(seeds[11], 1), TOKENS_B // TOKB)
    route_ids_turns = jax.random.permutation(jax.random.fold_in(seeds[11], 3), TOKENS_B // TOKB)
    route_ids = jax.vmap(lambda own, number: assign_block(jax.random.fold_in(seeds[11], 2), own, number, TOKB, EXPERTS, TOP, CAP, 1))(route_ids_keys, route_ids_turns).reshape((TOKENS_B, TOP))
    route_weights = jnp.clip(0.1 + 0.9 * jax.random.uniform(seeds[12], (TOKENS_B, TOP), jnp.float32) ** levels(seeds[12], (TOKENS_B, TOP), ((0, 64),), -0.2, 0.2), 0.1, 1.0)
    gate_weight = scatter_about(seeds[13], (EXPERTS, D, FE), D ** -0.5, 0.125, ((0, 64), (2, 4)))
    up_weight = scatter_about(seeds[14], (EXPERTS, D, FE), D ** -0.5, 0.125, ((0, 64), (2, 4)))
    down_weight = scatter_about(seeds[15], (EXPERTS, FE, D), FE ** -0.5, 0.1875, ((0, 64), (1, 4)))
    shared_gate = scatter_about(seeds[16], (D, FS), D ** -0.5, 0.125, ((1, 4),))
    shared_up = scatter_about(seeds[17], (D, FS), D ** -0.5, 0.125, ((1, 4),))
    shared_down = scatter_about(seeds[18], (FS, D), FS ** -0.5, 0.25, ((0, 4),))
    return {"query_latent": query_latent, "keyval_latent": keyval_latent, "rotary_key": rotary_key, "query_gain": query_gain, "keyval_gain": keyval_gain, "query_weight": query_weight, "keyval_weight": keyval_weight, "output_weight": output_weight, "output_gain": output_gain, "second_rows": second_rows, "second_gain": second_gain, "route_ids": route_ids, "route_weights": route_weights, "gate_weight": gate_weight, "up_weight": up_weight, "down_weight": down_weight, "shared_gate": shared_gate, "shared_up": shared_up, "shared_down": shared_down}


EPS = 1e-06
ROPE_BASE = 10000.0

def rms_scale(values, gain_vec):
    widened = values.astype(jnp.float32)
    normed = widened * lax.rsqrt(lax.optimization_barrier(jnp.mean(widened * widened, -1, keepdims=True)) + EPS)
    return (normed * gain_vec.astype(jnp.float32)).astype(jnp.bfloat16)

def rotate(values, positions):
    half_width = values.shape[-1] // 2
    inverse = 1.0 / ROPE_BASE ** (jnp.arange(half_width, dtype=jnp.float32) * 2.0 / (2 * half_width))
    angles = positions[:, None] * inverse[None, :]
    cosine = jnp.cos(angles)
    sine_vals = jnp.sin(angles)
    if values.ndim == 3:
        cosine = cosine[:, None, :]
        sine_vals = sine_vals[:, None, :]
    first_half = values[..., :half_width]
    second = values[..., half_width:]
    return jnp.concatenate([first_half * cosine - second * sine_vals, first_half * sine_vals + second * cosine], -1)

def round_trip(values):
    return lax.optimization_barrier(values.astype(jnp.bfloat16)).astype(jnp.float32)

def attention_part(query_latent, keyval_latent, rotary_key, query_gain, keyval_gain, query_weight, keyval_weight, output_weight, output_gain):
    positions = jnp.arange(SEQ, dtype=jnp.float32)
    queries = jnp.dot(rms_scale(query_latent, query_gain), query_weight, preferred_element_type=jnp.float32).reshape(SEQ, HEADS, NOPE + ROPE)
    queries = jnp.concatenate([queries[..., :NOPE], rotate(queries[..., NOPE:], positions)], -1).astype(jnp.bfloat16)
    keyvals = jnp.dot(rms_scale(keyval_latent, keyval_gain), keyval_weight, preferred_element_type=jnp.float32).astype(jnp.bfloat16)
    keyvals = keyvals.reshape(SEQ, HEADS, NOPE + VDIM)
    key_rot = rotate(rotary_key.astype(jnp.float32), positions).astype(jnp.bfloat16)
    key_plain = keyvals[..., :NOPE].astype(jnp.float32)
    values_all = keyvals[..., NOPE:].astype(jnp.float32)
    key_rot_wide = key_rot.astype(jnp.float32)
    score_scale = (NOPE + ROPE) ** (-0.5)
    block_rows = math.gcd(SEQ, 512)
    blocks = queries.reshape(SEQ // block_rows, block_rows, HEADS, NOPE + ROPE)

    def attend(query_block):
        query_wide = query_block.astype(jnp.float32)
        scores = jnp.einsum('qhd,khd->hqk', query_wide[..., :NOPE], key_plain)
        scores = (scores + jnp.einsum('qhr,kr->hqk', query_wide[..., NOPE:], key_rot_wide)) * score_scale
        top_score = lax.optimization_barrier(jnp.max(scores, -1, keepdims=True))
        exponent = jnp.exp(scores - top_score)
        denominator = lax.optimization_barrier(jnp.sum(exponent, -1))
        summed = jnp.einsum('hqk,khe->qhe', round_trip(exponent), values_all)
        return (summed / denominator.T[..., None]).astype(jnp.bfloat16)
    attended = lax.map(attend, blocks).reshape(SEQ, HEADS * VDIM)
    group_cols = HEADS * VDIM // N_TP
    mixture = jnp.zeros((SEQ, D), jnp.float32)
    for group_idx in range(N_TP):
        lower = group_idx * group_cols
        partial_value = jnp.dot(attended[:, lower:lower + group_cols], output_weight[lower:lower + group_cols], preferred_element_type=jnp.float32)
        mixture = mixture + round_trip(partial_value)
    return rms_scale(mixture, output_gain)

def grouped_down(hidden, down_mat, width):
    group_width = width // N_TP
    output = jnp.zeros((hidden.shape[0], down_mat.shape[1]), jnp.float32)
    for group_idx in range(N_TP):
        lower = group_idx * group_width
        partial_value = jnp.dot(hidden[:, lower:lower + group_width], down_mat[lower:lower + group_width], preferred_element_type=jnp.float32)
        output = output + round_trip(partial_value)
    return output

def expert_part(second_rows, second_gain, route_ids, route_weights, gate_weight, up_weight, down_weight, shared_gate, shared_up, shared_down):
    normed = rms_scale(second_rows, second_gain)
    padded = jnp.concatenate([normed, jnp.zeros((1, D), jnp.bfloat16)], 0)
    block_ids = route_ids.reshape(N_EP, TOKB * TOP)
    onehot = (block_ids[:, :, None] == jnp.arange(EXPERTS, dtype=jnp.int32)[None, None, :]).astype(jnp.int32)
    slot_rank = lax.optimization_barrier(jnp.sum((jnp.cumsum(onehot, 1) - 1) * onehot, 2))
    owners = (jnp.arange(N_EP * TOKB * TOP, dtype=jnp.int32) // TOP).reshape(N_EP, TOKB * TOP)
    sources = jnp.arange(N_EP, dtype=jnp.int32)[:, None]
    target = ((block_ids * N_EP + sources) * CAP + slot_rank).reshape(-1)
    slot_table = jnp.full((EXPERTS * N_EP * CAP,), N_EP * TOKB, jnp.int32).at[target].set(owners.reshape(-1))

    def run_expert(operands):
        gate_mat, up_mat, down_mat, rows_index = operands
        inputs = padded[rows_index]
        gate_act = jnp.dot(inputs, gate_mat, preferred_element_type=jnp.float32)
        up_act = jnp.dot(inputs, up_mat, preferred_element_type=jnp.float32)
        hidden = (jax.nn.silu(gate_act) * up_act).astype(jnp.bfloat16)
        return grouped_down(hidden, down_mat, FE).astype(jnp.bfloat16)
    expert_out = lax.map(run_expert, (gate_weight, up_weight, down_weight, slot_table.reshape(EXPERTS, N_EP * CAP)))
    expert_out = expert_out.reshape(EXPERTS * N_EP * CAP, D)
    picked = expert_out[target].astype(jnp.float32).reshape(N_EP * TOKB, TOP, D)
    routed = lax.optimization_barrier(jnp.sum(picked * route_weights.astype(jnp.float32)[:, :, None], 1))
    shared_hidden = (jax.nn.silu(jnp.dot(normed, shared_gate, preferred_element_type=jnp.float32)) * jnp.dot(normed, shared_up, preferred_element_type=jnp.float32)).astype(jnp.bfloat16)
    shared_out = grouped_down(shared_hidden, shared_down, FS)
    return (routed + shared_out).astype(jnp.bfloat16)

def reference(query_latent, keyval_latent, rotary_key, query_gain, keyval_gain, query_weight, keyval_weight, output_weight, output_gain, second_rows, second_gain, route_ids, route_weights, gate_weight, up_weight, down_weight, shared_gate, shared_up, shared_down):
    mixed = attention_part(query_latent, keyval_latent, rotary_key, query_gain, keyval_gain, query_weight, keyval_weight, output_weight, output_gain)
    expert_mix = expert_part(second_rows, second_gain, route_ids, route_weights, gate_weight, up_weight, down_weight, shared_gate, shared_up, shared_down)
    return (mixed, expert_mix)
```

```python
import functools

import jax
import jax.numpy as jnp
from jax import lax
from jax.experimental import pallas as pl
from jax.experimental.pallas import tpu as pltpu
from jax.sharding import PartitionSpec as P

NOPE = 64
ROPE = 32
VDIM = 64
EPS = 1e-06
ROPE_BASE = 10000.0
MESH = pl.DeviceIdType.MESH
F32 = jnp.float32
BF16 = jnp.bfloat16


def rms_scale(values, gain_vec):
    widened = values.astype(jnp.float32)
    normed = widened * lax.rsqrt(jnp.mean(widened * widened, -1, keepdims=True) + EPS)
    return (normed * gain_vec).astype(jnp.bfloat16)


def rotate(values, positions):
    half_width = values.shape[-1] // 2
    inverse = 1.0 / ROPE_BASE ** (
        jnp.arange(half_width, dtype=jnp.float32) * 2.0 / (2 * half_width)
    )
    angles = positions[:, None] * inverse[None, :]
    cosine = jnp.cos(angles)
    sine_vals = jnp.sin(angles)
    if values.ndim == 3:
        cosine = cosine[:, None, :]
        sine_vals = sine_vals[:, None, :]
    first_half = values[..., :half_width]
    second = values[..., half_width:]
    return jnp.concatenate(
        [first_half * cosine - second * sine_vals, first_half * sine_vals + second * cosine], -1
    )


def cut_along(shard, dim, size):
    lengths = shard.shape
    pieces = shard.reshape(*lengths[:dim], size, lengths[dim] // size, *lengths[dim + 1 :])
    return jnp.moveaxis(pieces, dim, 0)


def sent_and_summed(shard, axis, dim):
    pieces = cut_along(shard, dim, lax.axis_size(axis))
    arrived = lax.all_to_all(pieces, axis, split_axis=0, concat_axis=0, tiled=True)
    return arrived.astype(jnp.float32).sum(axis=0)


def mm(a, b):
    return jnp.dot(a, b, preferred_element_type=F32)


def iota(shape, dim):
    return lax.broadcasted_iota(jnp.int32, shape, dim)


NCH = 8
ROWS = 128
COLS = 512


def moe_kernel(
    rows_ref, gain_ref, ids_ref, idst_ref, w_ref,
    wg_hbm, wu_hbm, wd_hbm, sg_hbm, su_hbm, sd_hbm,
    out_ref,
    nrm, outq, wg, wu, wd, sg, su, sd, chi, clo,
    held, part, rly, fin, ret, back, acc,
    w_sem, disp_send, disp_recv, ag_send, agr, agl, agrr, agrl,
    rs_send, rlyr, rlyl, finr, finl, ret_send, ret_recv,
):
    e = lax.axis_index("ep")
    t = lax.axis_index("tp")
    z = e // 8
    k0 = e % 8
    right = (t + 1) % 4
    left = (t + 3) % 4
    opp = (t + 2) % 4

    barrier = pltpu.get_barrier_semaphore()

    def greet(j, _):
        pl.semaphore_signal(
            barrier, inc=1, device_id={"ep": (e + j) % 64, "tp": t}, device_id_type=MESH
        )
        return 0

    lax.fori_loop(1, 64, greet, 0)
    for other in (right, left):
        pl.semaphore_signal(barrier, inc=1, device_id={"ep": e, "tp": other}, device_id_type=MESH)

    loads = [
        pltpu.make_async_copy(src, dst, w_sem.at[n])
        for n, (src, dst) in enumerate(
            ((sg_hbm, sg), (su_hbm, su), (sd_hbm, sd), (wg_hbm, wg), (wu_hbm, wu), (wd_hbm, wd))
        )
    ]
    for load in loads:
        load.start()

    x = rows_ref[...].astype(F32)
    scale = lax.rsqrt(jnp.mean(x * x, -1, keepdims=True) + EPS)
    nrm[...] = (x * scale * gain_ref[...]).astype(BF16)

    idst = idst_ref[...]
    member_t = jnp.zeros((64, ROWS), F32)
    for k in range(4):
        member_t = member_t + jnp.where(idst[k : k + 1, :] == iota((64, ROWS), 0), 1.0, 0.0)
    before = jnp.where(iota((ROWS, ROWS), 0) < iota((ROWS, ROWS), 1), 1.0, 0.0).astype(BF16)
    place_t = (member_t * (mm(member_t.astype(BF16), before) + 1.0)).astype(BF16)
    spread_t = jnp.where((iota((1024, 64), 0) >> 4) == iota((1024, 64), 1), 1.0, 0.0).astype(BF16)
    slot_t = ((iota((1024, ROWS), 0) & 15) + 1).astype(F32)
    pick = jnp.where(mm(spread_t, place_t) == slot_t, 1.0, 0.0).astype(BF16)
    own_cols = pl.ds(pl.multiple_of(t * COLS, COLS), COLS)
    outq[...] = mm(pick, nrm[:, own_cols]).astype(BF16)

    pl.semaphore_wait(barrier, 65)

    def rows16(k):
        return pl.ds(pl.multiple_of(k * 16, 16), 16)

    def dispatch(n, _):
        i, k = n // 8, n % 8
        dest = ((z + 8 - i) % 8) * 8 + k

        @pl.when(dest != e)
        def _():
            pltpu.make_async_remote_copy(
                src_ref=outq.at[rows16(dest)],
                dst_ref=held.at[i, t, rows16(k0)],
                send_sem=disp_send,
                recv_sem=disp_recv.at[i],
                device_id={"ep": dest, "tp": t},
                device_id_type=MESH,
            ).start()

        return 0

    lax.fori_loop(0, 64, dispatch, 0)
    held[0, t, rows16(k0)] = outq[rows16(e)]

    ids = ids_ref[...]
    wts = w_ref[...]
    member = jnp.zeros((ROWS, 64), F32)
    weight = jnp.zeros((ROWS, 64), F32)
    for k in range(4):
        hit = ids[:, k : k + 1] == iota((ROWS, 64), 1)
        member = member + jnp.where(hit, 1.0, 0.0)
        weight = weight + jnp.where(hit, wts[:, k : k + 1], 0.0)
    after = jnp.where(iota((ROWS, ROWS), 0) > iota((ROWS, ROWS), 1), 1.0, 0.0).astype(BF16)
    place = (member * (mm(after, member.astype(BF16)) + 1.0)).astype(BF16)
    spread = jnp.where((iota((64, 1024), 1) >> 4) == iota((64, 1024), 0), 1.0, 0.0).astype(BF16)
    slot = ((iota((ROWS, 1024), 1) & 15) + 1).astype(F32)
    chosen = mm(place, spread) == slot
    high = weight.astype(BF16)
    low = (weight - high.astype(F32)).astype(BF16)
    chi[...] = jnp.where(chosen, mm(high, spread), 0.0).astype(BF16)
    clo[...] = jnp.where(chosen, mm(low, spread), 0.0).astype(BF16)

    def side(src, dst, send_sem, recv_sem, other):
        return pltpu.make_async_remote_copy(
            src_ref=src, dst_ref=dst, send_sem=send_sem, recv_sem=recv_sem,
            device_id={"ep": e, "tp": other}, device_id_type=MESH,
        )

    lo_half = pl.ds(0, 64)
    hi_half = pl.ds(64, 64)

    def scatter_first(n):
        side(part.at[n, opp, lo_half], rly.at[n, 0], rs_send, rlyr.at[n], right).start()
        side(part.at[n, opp, hi_half], rly.at[n, 1], rs_send, rlyl.at[n], left).start()
        side(part.at[n, right, hi_half], fin.at[n, 0, hi_half], rs_send, finr.at[n], right).start()
        side(part.at[n, left, lo_half], fin.at[n, 1, lo_half], rs_send, finl.at[n], left).start()

    def scatter_second(n):
        side(rly.at[n, 0], rly.at[n, 0], rs_send, rlyr.at[n], right).wait_recv()
        part[n, right, lo_half] = (
            part[n, right, lo_half].astype(F32) + rly[n, 0].astype(F32)
        ).astype(BF16)
        side(part.at[n, right, lo_half], fin.at[n, 0, lo_half], rs_send, finr.at[n], right).start()
        side(rly.at[n, 1], rly.at[n, 1], rs_send, rlyl.at[n], left).wait_recv()
        part[n, left, hi_half] = (
            part[n, left, hi_half].astype(F32) + rly[n, 1].astype(F32)
        ).astype(BF16)
        side(part.at[n, left, hi_half], fin.at[n, 1, hi_half], rs_send, finl.at[n], left).start()

    def scatter_last(n):
        side(fin.at[n, 0], fin.at[n, 0], rs_send, finr.at[n], right).wait_recv()
        side(fin.at[n, 1], fin.at[n, 1], rs_send, finl.at[n], left).wait_recv()
        return part[n, t].astype(F32) + fin[n, 0].astype(F32) + fin[n, 1].astype(F32)

    def swish(g, u):
        return (g / (1.0 + jnp.exp(-g)) * u).astype(BF16)

    for load in loads[:3]:
        load.wait()
    shared = swish(mm(nrm[...], sg[...]), mm(nrm[...], su[...]))
    for q in range(4):
        part[NCH, q] = mm(shared, sd[:, q * COLS : (q + 1) * COLS]).astype(BF16)
    scatter_first(NCH)
    for load in loads[3:]:
        load.wait()

    acc[...] = jnp.zeros_like(acc)

    def arrive(i):
        @pl.when(i == 0)
        def _():
            some = held.at[0, t, pl.ds(0, 112)]
            side(some, some, disp_send, disp_recv.at[0], right).wait_recv()

        @pl.when(i > 0)
        def _():
            whole = held.at[i, t]
            side(whole, whole, disp_send, disp_recv.at[i], right).wait_recv()

        side(held.at[i, t], held.at[i, t], ag_send, agr.at[i], right).start()
        side(held.at[i, t], held.at[i, t], ag_send, agl.at[i], left).start()

    def pass_on(i):
        side(held.at[i, left], held.at[i, left], ag_send, agr.at[i], right).wait_recv()
        side(
            held.at[i, left, lo_half], held.at[i, left, lo_half], ag_send, agrr.at[i], right
        ).start()
        side(held.at[i, right], held.at[i, right], ag_send, agl.at[i], left).wait_recv()
        side(
            held.at[i, right, hi_half], held.at[i, right, hi_half], ag_send, agrl.at[i], left
        ).start()

    def expert(i):
        side(
            held.at[i, opp, lo_half], held.at[i, opp, lo_half], ag_send, agrr.at[i], right
        ).wait_recv()
        side(
            held.at[i, opp, hi_half], held.at[i, opp, hi_half], ag_send, agrl.at[i], left
        ).wait_recv()
        g = jnp.zeros((ROWS, 256), F32)
        u = jnp.zeros((ROWS, 256), F32)
        for q in range(4):
            piece = held[i, q]
            g = g + mm(piece, wg[q * COLS : (q + 1) * COLS, :])
            u = u + mm(piece, wu[q * COLS : (q + 1) * COLS, :])
        hidden = swish(g, u)
        for q in range(4):
            part[i, q] = mm(hidden, wd[:, q * COLS : (q + 1) * COLS]).astype(BF16)
        scatter_first(i)

    def give_back(i):
        ret[i] = scatter_last(i).astype(BF16)

        def one(k, _):
            dest = ((z + i) % 8) * 8 + k

            @pl.when(dest != e)
            def _():
                pltpu.make_async_remote_copy(
                    src_ref=ret.at[i, rows16(k)],
                    dst_ref=back.at[i, rows16(k0)],
                    send_sem=ret_send,
                    recv_sem=ret_recv.at[i],
                    device_id={"ep": dest, "tp": t},
                    device_id_type=MESH,
                ).start()

            return 0

        lax.fori_loop(0, 8, one, 0)

        @pl.when(i == 0)
        def _():
            back[0, rows16(k0)] = ret[0, rows16(k0)]

    def combine(i):
        @pl.when(i == 0)
        def _():
            some = back.at[0, pl.ds(0, 112)]
            side(some, some, ret_send, ret_recv.at[0], right).wait_recv()

        @pl.when(i > 0)
        def _():
            side(back.at[i], back.at[i], ret_send, ret_recv.at[i], right).wait_recv()

        cols = pl.ds(pl.multiple_of(((z + 8 - i) % 8) * 128, 128), 128)
        acc[...] += mm(chi[:, cols], back[i]) + mm(clo[:, cols], back[i])

    def step(j, _):
        for stage, lag in (
            (arrive, 0), (pass_on, 1), (expert, 2), (scatter_second, 3), (give_back, 4), (combine, 5)
        ):
            @pl.when(jnp.logical_and(j >= lag, j < lag + NCH))
            def _(stage=stage, lag=lag):
                stage(j - lag)

        @pl.when(j == 1)
        def _():
            scatter_second(NCH)

        @pl.when(j == 3)
        def _():
            acc[...] += scatter_last(NCH)

        return 0

    lax.fori_loop(0, NCH + 5, step, 0)
    out_ref[...] = acc[...].astype(BF16)

    sent = outq.at[pl.ds(0, 1008)]
    side(sent, sent, disp_send, disp_recv.at[0], right).wait_send()

    def drain(i, _):
        for piece in (held.at[i, 0], held.at[i, 0], held.at[i, 0]):
            side(piece, piece, ag_send, agr.at[0], right).wait_send()
        return 0

    lax.fori_loop(0, NCH, drain, 0)

    def drain_rs(n, _):
        for piece in (part.at[n, 0], part.at[n, 0], part.at[n, 0]):
            side(piece, piece, rs_send, finr.at[0], right).wait_send()
        return 0

    lax.fori_loop(0, NCH + 1, drain_rs, 0)
    for i in range(NCH):
        piece = ret.at[i, pl.ds(0, 112 if i == 0 else 128)]
        side(piece, piece, ret_send, ret_recv.at[0], right).wait_send()


def moe(rows, gain, ids, wts, wg, wu, wd, sg, su, sd):
    vm = pl.BlockSpec(memory_space=pltpu.VMEM)
    anym = pl.BlockSpec(memory_space=pl.ANY)
    dma = pltpu.SemaphoreType.DMA
    return pl.pallas_call(
        moe_kernel,
        name="moe",
        out_shape=jax.ShapeDtypeStruct((ROWS, COLS), BF16),
        in_specs=[vm] * 5 + [anym] * 6,
        out_specs=vm,
        scratch_shapes=[
            pltpu.VMEM((ROWS, 2048), BF16),
            pltpu.VMEM((1024, COLS), BF16),
            pltpu.VMEM((2048, 256), BF16),
            pltpu.VMEM((2048, 256), BF16),
            pltpu.VMEM((256, 2048), BF16),
            pltpu.VMEM((2048, 128), BF16),
            pltpu.VMEM((2048, 128), BF16),
            pltpu.VMEM((128, 2048), BF16),
            pltpu.VMEM((ROWS, 1024), BF16),
            pltpu.VMEM((ROWS, 1024), BF16),
            pltpu.VMEM((NCH, 4, ROWS, COLS), BF16),
            pltpu.VMEM((NCH + 1, 4, ROWS, COLS), BF16),
            pltpu.VMEM((NCH + 1, 2, 64, COLS), BF16),
            pltpu.VMEM((NCH + 1, 2, ROWS, COLS), BF16),
            pltpu.VMEM((NCH, ROWS, COLS), BF16),
            pltpu.VMEM((NCH, ROWS, COLS), BF16),
            pltpu.VMEM((ROWS, COLS), F32),
            dma((6,)),
            dma, dma((NCH,)),
            dma, dma((NCH,)), dma((NCH,)), dma((NCH,)), dma((NCH,)),
            dma, dma((NCH + 1,)), dma((NCH + 1,)), dma((NCH + 1,)), dma((NCH + 1,)),
            dma, dma((NCH,)),
        ],
        compiler_params=pltpu.CompilerParams(
            collective_id=0, has_side_effects=True, vmem_limit_bytes=56 * 1024 * 1024
        ),
        cost_estimate=pl.CostEstimate(flops=80_000_000_000, bytes_accessed=8_000_000, transcendentals=0),
    )(rows, gain.reshape(1, -1), ids, ids.T, wts, wg, wu, wd, sg, su, sd)


def per_device(
    query_latent, keyval_latent, rotary_key, query_gain, keyval_gain, query_weight, keyval_weight,
    output_weight, output_gain, second_rows, second_gain, route_ids, route_weights,
    gate_weight, up_weight, down_weight, shared_gate, shared_up, shared_down,
):
    first_rows = query_latent.shape[0]
    head_count = query_weight.shape[1] // (NOPE + ROPE)
    positions = (lax.axis_index("ep") * first_rows).astype(jnp.float32) + jnp.arange(
        first_rows, dtype=jnp.float32
    )
    queries = jnp.dot(
        rms_scale(query_latent, query_gain), query_weight, preferred_element_type=jnp.float32
    ).reshape(first_rows, head_count, NOPE + ROPE)
    queries = jnp.concatenate(
        [queries[..., :NOPE], rotate(queries[..., NOPE:], positions)], -1
    ).astype(jnp.bfloat16)
    query_plain = queries[..., :NOPE]
    query_turned = queries[..., NOPE:]
    kv_normed = rms_scale(keyval_latent, keyval_gain)
    key_rot = rotate(rotary_key.astype(jnp.float32), positions).astype(jnp.bfloat16)
    score_scale = (NOPE + ROPE) ** (-0.5)
    keyvals = jnp.dot(kv_normed, keyval_weight, preferred_element_type=jnp.float32).astype(
        jnp.bfloat16
    )
    both = lax.all_gather(jnp.concatenate([keyvals, key_rot], 1), "ep", axis=0, tiled=True)
    expert_mix = moe(
        second_rows, second_gain, route_ids, route_weights,
        gate_weight[0], up_weight[0], down_weight[0], shared_gate, shared_up, shared_down,
    )
    keyval_piece = both[:, : keyvals.shape[1]]
    rot_piece = both[:, keyvals.shape[1] :]
    keyval_heads = keyval_piece.reshape(-1, head_count, NOPE + VDIM)
    scores = jnp.einsum(
        "qhd,khd->hqk", query_plain, keyval_heads[..., :NOPE], preferred_element_type=jnp.float32
    )
    scores = (
        scores
        + jnp.einsum("qhr,kr->hqk", query_turned, rot_piece, preferred_element_type=jnp.float32)
    ) * score_scale
    new_high = jnp.max(scores, -1)
    exponent = jnp.exp(scores - new_high[..., None])
    denominator = jnp.sum(exponent, -1)
    accumulated = jnp.einsum(
        "hqk,khe->qhe",
        exponent.astype(jnp.bfloat16),
        keyval_heads[..., NOPE:],
        preferred_element_type=jnp.float32,
    )
    attended = (
        (accumulated / denominator.T[..., None])
        .astype(jnp.bfloat16)
        .reshape(first_rows, head_count * VDIM)
    )
    mixture = sent_and_summed(
        jnp.dot(attended, output_weight, preferred_element_type=jnp.float32).astype(jnp.bfloat16),
        "tp",
        0,
    )
    mixed = rms_scale(mixture, output_gain)
    return (mixed, expert_mix)


def solution(mesh):
    placed = (
        P("ep", None), P("ep", None), P("ep", None), P(), P(), P(None, "tp"), P(None, "tp"),
        P("tp", None), P(), P("ep", None), P(), P("ep", None), P("ep", None),
        P("ep", None, "tp"), P("ep", None, "tp"), P("ep", "tp", None),
        P(None, "tp"), P(None, "tp"), P("tp", None),
    )
    return jax.shard_map(
        per_device,
        mesh=mesh,
        in_specs=placed,
        out_specs=(P(("ep", "tp"), None), P("ep", "tp")),
        check_vma=False,
    )
```

```python
import functools

import jax
import jax.numpy as jnp
from jax import lax
from jax.experimental import pallas as pl
from jax.experimental.pallas import tpu as pltpu
from jax.sharding import PartitionSpec as P

NOPE = 64
ROPE = 32
VDIM = 64
EPS = 1e-06
ROPE_BASE = 10000.0
MESH = pl.DeviceIdType.MESH
F32 = jnp.float32
BF16 = jnp.bfloat16


def mm(a, b):
    return jnp.dot(a, b, preferred_element_type=F32)


def mm_t(a, b):
    return lax.dot_general(a, b, (((0,), (0,)), ((), ())), preferred_element_type=F32)


def mm_nt(a, b):
    return lax.dot_general(a, b, (((1,), (1,)), ((), ())), preferred_element_type=F32)


def iota(shape, dim):
    return lax.broadcasted_iota(jnp.int32, shape, dim)


def normalized(x, gain):
    return x * lax.rsqrt(jnp.mean(x * x, -1, keepdims=True) + EPS) * gain


def parts3(x):
    a = x.astype(BF16)
    b = (x - a.astype(F32)).astype(BF16)
    c = (x - a.astype(F32) - b.astype(F32)).astype(BF16)
    return a, b, c


NCH = 8
ROWS = 128
COLS = 512
KVW = 640
FACTOR = 1.4426950408889634 * (NOPE + ROPE) ** -0.5


def moe_kernel(
    rows_ref, gain_ref, idst_ref, wt_ref,
    ql_ref, qgain_ref, kl_ref, kgain_ref, rk_ref, cos_ref, sin_ref, ogain_ref,
    wkv_hbm, sg_hbm, su_hbm, sd_hbm, wq_hbm, wg_hbm, wu_hbm, wd_hbm, wo_hbm,
    mix_ref, out_ref,
    nrm, outq, wkv, sg, su, sd, wq, wg, wu, wd, wo, pick, chi, clo,
    held, part, rly, fin, ret, back, acc,
    kvall, qall, scores, half, other_half,
    w_sem, kv_send, kzr, kzl, kyr, kyl, kyx, q_send, q_recv, half_send, half_recv,
    disp_send, disp_recv, ag_send, agr, agl, agrr, agrl,
    rs_send, rlyr, rlyl, finr, finl, ret_send, ret_recv,
):
    e = lax.axis_index("ep")
    t = lax.axis_index("tp")
    z = e // 8
    k0 = e % 8
    right = (t + 1) % 4
    left = (t + 3) % 4
    opp = (t + 2) % 4
    y = (e // 2) % 4
    core = e % 2
    z_up, z_down = (e + 8) % 64, (e + 56) % 64
    y_up = z * 8 + ((y + 1) % 4) * 2 + core
    y_down = z * 8 + ((y + 3) % 4) * 2 + core
    mate = e + 1 - 2 * core

    barrier = pltpu.get_barrier_semaphore()

    def greet(j, _):
        pl.semaphore_signal(
            barrier, inc=1, device_id={"ep": (e + j) % 64, "tp": t}, device_id_type=MESH
        )
        return 0

    lax.fori_loop(1, 64, greet, 0)
    for other in (right, left):
        pl.semaphore_signal(barrier, inc=1, device_id={"ep": e, "tp": other}, device_id_type=MESH)

    pairs = (
        (wkv_hbm, wkv), (sg_hbm, sg), (su_hbm, su), (sd_hbm, sd), (wq_hbm, wq),
        (wg_hbm, wg), (wu_hbm, wu), (wd_hbm, wd),
    ) + tuple((wo_hbm.at[pl.ds(64 * h, 64)], wo.at[h, pl.ds(64, 64)]) for h in range(4))
    loads = [
        pltpu.make_async_copy(src, dst, w_sem.at[n]) for n, (src, dst) in enumerate(pairs)
    ]
    for load in loads:
        load.start()

    nrm[...] = normalized(rows_ref[...].astype(F32), gain_ref[...]).astype(BF16)

    idst = idst_ref[...]
    member = jnp.zeros((64, ROWS), F32)
    for k in range(4):
        member = member + jnp.where(idst[k : k + 1, :] == iota((64, ROWS), 0), 1.0, 0.0)
    before = jnp.where(iota((ROWS, ROWS), 0) < iota((ROWS, ROWS), 1), 1.0, 0.0).astype(BF16)
    place = (member * (mm(member.astype(BF16), before) + 1.0)).astype(BF16)
    spread = jnp.where((iota((1024, 64), 0) >> 4) == iota((1024, 64), 1), 1.0, 0.0).astype(BF16)
    slot = ((iota((1024, ROWS), 0) & 15) + 1).astype(F32)
    pick[...] = jnp.where(mm(spread, place) == slot, 1.0, 0.0).astype(BF16)
    own_cols = pl.ds(pl.multiple_of(t * COLS, COLS), COLS)
    outq[...] = mm(pick[...], nrm[:, own_cols]).astype(BF16)

    lane = iota((16, ROWS), 1)
    expand = jnp.where(
        jnp.logical_and((lane & 15) == iota((16, ROWS), 0), lane < 32), 1.0, 0.0
    ).astype(BF16)
    cosine = sum(mm_t(p, expand) for p in parts3(cos_ref[...]))
    sine = sum(mm_t(p, expand) for p in parts3(sin_ref[...]))
    sine = jnp.where(iota((ROWS, ROWS), 1) < 16, -sine, sine)

    straight = jnp.where(iota((32, ROWS), 0) == iota((32, ROWS), 1), 1.0, 0.0).astype(BF16)
    swapped = jnp.where(iota((32, ROWS), 0) == (iota((32, ROWS), 1) ^ 16), 1.0, 0.0).astype(BF16)
    rk = rk_ref[...]
    kvall[y, z, :, 512:] = (mm_t(rk, straight) * cosine + mm_t(rk, swapped) * sine).astype(BF16)
    loads[0].wait()
    kvn = normalized(kl_ref[...].astype(F32), kgain_ref[...]).astype(BF16)
    kvall[y, z, :, :512] = mm(kvn, wkv[...]).astype(BF16)

    pl.semaphore_wait(barrier, 65)

    def rows16(k):
        return pl.ds(pl.multiple_of(k * 16, 16), 16)

    def along_ep(src, dst, send_sem, recv_sem, dest):
        return pltpu.make_async_remote_copy(
            src_ref=src, dst_ref=dst, send_sem=send_sem, recv_sem=recv_sem,
            device_id={"ep": dest, "tp": t}, device_id_type=MESH,
        )

    def kv_copy(yi, o, recv_sem, dest):
        block = kvall.at[yi, (z + 8 - o) % 8]
        return along_ep(block, block, kv_send, recv_sem, dest)

    def kv_sideways(o):
        kv_copy(y, o, kyr.at[o], y_up).start()
        kv_copy(y, o, kyl.at[o], y_down).start()

    kv_copy(y, 0, kzr.at[0], z_up).start()
    kv_copy(y, 0, kzl.at[0], z_down).start()
    kv_sideways(0)

    def dispatch(i):
        def one(k, _):
            dest = ((z + 8 - i) % 8) * 8 + k

            @pl.when(dest != e)
            def _():
                along_ep(
                    outq.at[rows16(dest)], held.at[i, t, rows16(k0)], disp_send, disp_recv.at[i], dest
                ).start()

            return 0

        lax.fori_loop(0, 8, one, 0)

    def dispatch_early(i, _):
        dispatch(i)
        return 0

    lax.fori_loop(0, 4, dispatch_early, 0)
    held[0, t, rows16(k0)] = outq[rows16(e)]

    def kv_ring(s):
        kv_copy(y, s + 1, kzr.at[s], z_up).wait_recv()
        if s < 3:
            kv_copy(y, s + 1, kzr.at[s + 1], z_up).start()
        kv_sideways(s + 1)
        if s < 3:
            kv_copy(y, 7 - s, kzl.at[s], z_down).wait_recv()
            if s < 2:
                kv_copy(y, 7 - s, kzl.at[s + 1], z_down).start()
            kv_sideways(7 - s)

    def kv_relay(r):
        for o in {r, (8 - r) % 8}:
            kv_copy((y + 3) % 4, o, kyr.at[o], y_up).wait_recv()
            kv_copy((y + 1) % 4, o, kyl.at[o], y_up).wait_recv()
            if 1 <= o <= 4:
                kv_copy((y + 3) % 4, o, kyx.at[o], y_up).start()
            else:
                kv_copy((y + 1) % 4, o, kyx.at[o], y_down).start()

    def kv_rest():
        for o in range(8):
            kv_copy((y + 2) % 4, o, kyx.at[o], y_up).wait_recv()

    def attend(h):
        cols = pl.ds(pl.multiple_of(h * 128, 128), 128)
        q = jnp.concatenate([qall[0, h], qall[1, h]], axis=0)

        def tile(n):
            yi, zs = n // 2, pl.ds((n % 2) * 4, 4)
            return kvall[yi, zs, :, cols].reshape(512, 128), kvall[yi, zs, :, 512:].reshape(512, 128)

        def first(n, high):
            plain, turned = tile(n)
            s = mm_nt(q, jnp.concatenate([plain, turned], axis=1))
            scores[n] = s
            for b in range(4):
                high = jnp.maximum(high, s[:, b * 128 : (b + 1) * 128])
            return high

        high = lax.fori_loop(0, 8, first, jnp.full((256, 128), -jnp.inf, F32))
        high = jnp.max(high, -1, keepdims=True)

        def second(n, carry):
            total, summed = carry
            p = jnp.exp2((scores[n] - high) * FACTOR)
            for b in range(4):
                total = total + p[:, b * 128 : (b + 1) * 128]
            return total, summed + mm(p.astype(BF16), tile(n)[0])

        zero = jnp.zeros((256, 128), F32)
        total, summed = lax.fori_loop(0, 8, second, (zero, zero))
        total = jnp.sum(total, -1, keepdims=True)
        ln = iota((256, 128), 1)
        summed = jnp.where(ln < 32, high, jnp.where(ln < 64, total, summed))
        half[0, h] = summed[:128]
        half[1, h] = summed[128:]
        along_ep(
            half.at[1 - core, h], other_half.at[h], half_send, half_recv.at[h], mate
        ).start()

    def project():
        head = jnp.zeros((ROWS, 2048), F32)
        ln = iota((ROWS, 128), 1)
        for h in range(4):
            along_ep(
                half.at[1 - core, h], other_half.at[h], half_send, half_recv.at[h], mate
            ).wait_recv()
            one, two = half[core, h], other_half[h]
            top = jnp.maximum(one[:, 0:1], two[:, 0:1])
            w1 = jnp.exp2((one[:, 0:1] - top) * FACTOR)
            w2 = jnp.exp2((two[:, 0:1] - top) * FACTOR)
            value = (one * w1 + two * w2) / (one[:, 32:33] * w1 + two[:, 32:33] * w2)
            value = jnp.where(ln < 64, 0.0, value).astype(BF16)
            head = head + mm(value, wo[h])
        head = head.astype(BF16)
        for q in range(4):
            for b in range(4):
                part[NCH + 1, q, 32 * b : 32 * b + 32] = head[
                    32 * q : 32 * q + 32, COLS * b : COLS * b + COLS
                ]
        scatter_first(NCH + 1)

    def finish_mix():
        mixture = scatter_last(NCH + 1)
        blocks = [mixture[32 * b : 32 * b + 32] for b in range(4)]
        square = sum(jnp.sum(v * v, -1, keepdims=True) for v in blocks) * (1.0 / 2048)
        scale = lax.rsqrt(square + EPS)
        for b in range(4):
            cols = slice(COLS * b, COLS * b + COLS)
            mix_ref[:, cols] = (blocks[b] * scale * ogain_ref[:, cols]).astype(BF16)

    def side(src, dst, send_sem, recv_sem, other):
        return pltpu.make_async_remote_copy(
            src_ref=src, dst_ref=dst, send_sem=send_sem, recv_sem=recv_sem,
            device_id={"ep": e, "tp": other}, device_id_type=MESH,
        )

    lo_half = pl.ds(0, 64)
    hi_half = pl.ds(64, 64)

    def scatter_first(n):
        side(part.at[n, opp, lo_half], rly.at[n, 0], rs_send, rlyr.at[n], right).start()
        side(part.at[n, opp, hi_half], rly.at[n, 1], rs_send, rlyl.at[n], left).start()
        side(part.at[n, right, hi_half], fin.at[n, 0, hi_half], rs_send, finr.at[n], right).start()
        side(part.at[n, left, lo_half], fin.at[n, 1, lo_half], rs_send, finl.at[n], left).start()

    def scatter_second(n):
        side(rly.at[n, 0], rly.at[n, 0], rs_send, rlyr.at[n], right).wait_recv()
        part[n, right, lo_half] = (
            part[n, right, lo_half].astype(F32) + rly[n, 0].astype(F32)
        ).astype(BF16)
        side(part.at[n, right, lo_half], fin.at[n, 0, lo_half], rs_send, finr.at[n], right).start()
        side(rly.at[n, 1], rly.at[n, 1], rs_send, rlyl.at[n], left).wait_recv()
        part[n, left, hi_half] = (
            part[n, left, hi_half].astype(F32) + rly[n, 1].astype(F32)
        ).astype(BF16)
        side(part.at[n, left, hi_half], fin.at[n, 1, hi_half], rs_send, finl.at[n], left).start()

    def scatter_last(n):
        side(fin.at[n, 0], fin.at[n, 0], rs_send, finr.at[n], right).wait_recv()
        side(fin.at[n, 1], fin.at[n, 1], rs_send, finl.at[n], left).wait_recv()
        return part[n, t].astype(F32) + fin[n, 0].astype(F32) + fin[n, 1].astype(F32)

    def swish(g, u):
        return (g / (1.0 + jnp.exp(-g)) * u).astype(BF16)

    for load in loads[1:4]:
        load.wait()
    shared = swish(mm(nrm[...], sg[...]), mm(nrm[...], su[...]))
    for q in range(4):
        part[NCH, q] = mm(shared, sd[:, q * COLS : (q + 1) * COLS]).astype(BF16)
    scatter_first(NCH)
    loads[4].wait()
    qn = normalized(ql_ref[...].astype(F32), qgain_ref[...]).astype(BF16)
    spot = iota((384, 384), 1)
    in_tile = spot & 127
    kind = spot >> 7
    for h in range(4):
        origin = jnp.where(kind == 0, in_tile, 64 + jnp.where(kind == 1, in_tile, in_tile ^ 16))
        valid = in_tile < jnp.where(kind == 0, 64, 32)
        select = jnp.where(
            jnp.logical_and(valid, iota((384, 384), 0) == origin + 96 * h), 1.0, 0.0
        ).astype(BF16)
        three = mm(qn, mm(wq[...], select).astype(BF16))
        qall[core, h, :, :128] = three[:, :128].astype(BF16)
        qall[core, h, :, 128:] = (three[:, 128:256] * cosine + three[:, 256:] * sine).astype(BF16)
    along_ep(qall.at[core], qall.at[core], q_send, q_recv, mate).start()

    wts = wt_ref[...]
    weight = jnp.zeros((64, ROWS), F32)
    for k in range(4):
        weight = weight + jnp.where(
            idst[k : k + 1, :] == iota((64, ROWS), 0), wts[k : k + 1, :], 0.0
        )
    high_part = weight.astype(BF16)
    low_part = (weight - high_part.astype(F32)).astype(BF16)
    chi[...] = (pick[...].astype(F32) * mm(spread, high_part)).astype(BF16)
    clo[...] = (pick[...].astype(F32) * mm(spread, low_part)).astype(BF16)
    wo[:, 0:64] = jnp.zeros((4, 64, 2048), BF16)

    for load in loads[5:]:
        load.wait()

    acc[...] = jnp.zeros_like(acc)

    def arrive(i):
        @pl.when(i == 0)
        def _():
            some = held.at[0, t, pl.ds(0, 112)]
            side(some, some, disp_send, disp_recv.at[0], right).wait_recv()

        @pl.when(i > 0)
        def _():
            whole = held.at[i, t]
            side(whole, whole, disp_send, disp_recv.at[i], right).wait_recv()

        side(held.at[i, t], held.at[i, t], ag_send, agr.at[i], right).start()
        side(held.at[i, t], held.at[i, t], ag_send, agl.at[i], left).start()

    def pass_on(i):
        side(held.at[i, left], held.at[i, left], ag_send, agr.at[i], right).wait_recv()
        side(
            held.at[i, left, lo_half], held.at[i, left, lo_half], ag_send, agrr.at[i], right
        ).start()
        side(held.at[i, right], held.at[i, right], ag_send, agl.at[i], left).wait_recv()
        side(
            held.at[i, right, hi_half], held.at[i, right, hi_half], ag_send, agrl.at[i], left
        ).start()

    def expert(i):
        side(
            held.at[i, opp, lo_half], held.at[i, opp, lo_half], ag_send, agrr.at[i], right
        ).wait_recv()
        side(
            held.at[i, opp, hi_half], held.at[i, opp, hi_half], ag_send, agrl.at[i], left
        ).wait_recv()
        g = jnp.zeros((ROWS, 256), F32)
        u = jnp.zeros((ROWS, 256), F32)
        for q in range(4):
            piece = held[i, q]
            g = g + mm(piece, wg[q * COLS : (q + 1) * COLS, :])
            u = u + mm(piece, wu[q * COLS : (q + 1) * COLS, :])
        hidden = swish(g, u)
        for q in range(4):
            part[i, q] = mm(hidden, wd[:, q * COLS : (q + 1) * COLS]).astype(BF16)
        scatter_first(i)

    def give_back(i):
        ret[i] = scatter_last(i).astype(BF16)

        def one(k, _):
            dest = ((z + i) % 8) * 8 + k

            @pl.when(dest != e)
            def _():
                pltpu.make_async_remote_copy(
                    src_ref=ret.at[i, rows16(k)],
                    dst_ref=back.at[i, rows16(k0)],
                    send_sem=ret_send,
                    recv_sem=ret_recv.at[i],
                    device_id={"ep": dest, "tp": t},
                    device_id_type=MESH,
                ).start()

            return 0

        lax.fori_loop(0, 8, one, 0)

        @pl.when(i == 0)
        def _():
            back[0, rows16(k0)] = ret[0, rows16(k0)]

    def combine(i):
        @pl.when(i == 0)
        def _():
            some = back.at[0, pl.ds(0, 112)]
            side(some, some, ret_send, ret_recv.at[0], right).wait_recv()

        @pl.when(i > 0)
        def _():
            side(back.at[i], back.at[i], ret_send, ret_recv.at[i], right).wait_recv()

        cols = pl.ds(pl.multiple_of(((z + 8 - i) % 8) * 128, 128), 128)
        acc[...] += mm_t(chi[cols, :], back[i]) + mm_t(clo[cols, :], back[i])

    def step(j, _):
        for stage, lag in (
            (arrive, 0), (pass_on, 1), (expert, 2), (scatter_second, 3), (give_back, 4), (combine, 5)
        ):
            @pl.when(jnp.logical_and(j >= lag, j < lag + NCH))
            def _(stage=stage, lag=lag):
                stage(j - lag)

        @pl.when(j == 1)
        def _():
            scatter_second(NCH)

        @pl.when(j == 3)
        def _():
            acc[...] += scatter_last(NCH)

        @pl.when(j < 4)
        def _():
            dispatch(j + 4)

        for s in range(4):
            @pl.when(j == s)
            def _(s=s):
                kv_ring(s)

        for r in range(5):
            @pl.when(j == r)
            def _(r=r):
                kv_relay(r)

        @pl.when(j == 6)
        def _():
            kv_rest()
            along_ep(qall.at[1 - core], qall.at[1 - core], q_send, q_recv, mate).wait_recv()

        @pl.when(jnp.logical_and(j >= 6, j < 10))
        def _():
            attend(j - 6)

        @pl.when(j == 10)
        def _():
            project()

        @pl.when(j == 11)
        def _():
            scatter_second(NCH + 1)

        @pl.when(j == 12)
        def _():
            finish_mix()

        return 0

    lax.fori_loop(0, NCH + 5, step, 0)
    out_ref[...] = acc[...].astype(BF16)

    sent = outq.at[pl.ds(0, 1008)]
    side(sent, sent, disp_send, disp_recv.at[0], right).wait_send()

    def drain(i, _):
        for piece in (held.at[i, 0], held.at[i, 0], held.at[i, 0]):
            side(piece, piece, ag_send, agr.at[0], right).wait_send()
        return 0

    lax.fori_loop(0, NCH, drain, 0)

    def drain_rs(n, _):
        for piece in (part.at[n, 0], part.at[n, 0], part.at[n, 0]):
            side(piece, piece, rs_send, finr.at[0], right).wait_send()
        return 0

    lax.fori_loop(0, NCH + 2, drain_rs, 0)
    for i in range(NCH):
        piece = ret.at[i, pl.ds(0, 112 if i == 0 else 128)]
        side(piece, piece, ret_send, ret_recv.at[0], right).wait_send()

    def drain_kv(n, _):
        kv_copy(y, 0, kzr.at[0], z_up).wait_send()
        return 0

    lax.fori_loop(0, 31, drain_kv, 0)
    along_ep(qall.at[core], qall.at[core], q_send, q_recv, mate).wait_send()
    along_ep(other_half, other_half, half_send, half_recv.at[0], mate).wait_send()


def fused(small, weights):
    vm = pl.BlockSpec(memory_space=pltpu.VMEM)
    anym = pl.BlockSpec(memory_space=pl.ANY)
    dma = pltpu.SemaphoreType.DMA

    def buf(*shape, dtype=BF16):
        return pltpu.VMEM(shape, dtype)

    return pl.pallas_call(
        moe_kernel,
        name="fused",
        out_shape=(
            jax.ShapeDtypeStruct((32, 2048), BF16),
            jax.ShapeDtypeStruct((ROWS, COLS), BF16),
        ),
        in_specs=[vm] * len(small) + [anym] * len(weights),
        out_specs=(vm, vm),
        scratch_shapes=[
            buf(ROWS, 2048), buf(1024, COLS),
            buf(512, 512), buf(2048, 128), buf(2048, 128), buf(128, 2048), buf(768, 384),
            buf(2048, 256), buf(2048, 256), buf(256, 2048), buf(4, 128, 2048),
            buf(1024, ROWS), buf(1024, ROWS), buf(1024, ROWS),
            buf(NCH, 4, ROWS, COLS), buf(NCH + 2, 4, ROWS, COLS), buf(NCH + 2, 2, 64, COLS),
            buf(NCH + 2, 2, ROWS, COLS), buf(NCH, ROWS, COLS), buf(NCH, ROWS, COLS),
            buf(ROWS, COLS, dtype=F32),
            buf(4, 8, ROWS, KVW), buf(2, 4, ROWS, 256), buf(8, 256, 512, dtype=F32),
            buf(2, 4, ROWS, 128, dtype=F32), buf(4, ROWS, 128, dtype=F32),
            dma((12,)), dma, dma((4,)), dma((4,)), dma((8,)), dma((8,)), dma((8,)),
            dma, dma, dma, dma((4,)),
            dma, dma((NCH,)),
            dma, dma((NCH,)), dma((NCH,)), dma((NCH,)), dma((NCH,)),
            dma, dma((NCH + 2,)), dma((NCH + 2,)), dma((NCH + 2,)), dma((NCH + 2,)),
            dma, dma((NCH,)),
        ],
        compiler_params=pltpu.CompilerParams(
            collective_id=0, has_side_effects=True, vmem_limit_bytes=56 * 1024 * 1024
        ),
        cost_estimate=pl.CostEstimate(flops=80_000_000_000, bytes_accessed=8_000_000, transcendentals=0),
    )(*small, *weights)


def per_device(
    query_latent, keyval_latent, rotary_key, query_gain, keyval_gain, query_weight, keyval_weight,
    output_weight, output_gain, second_rows, second_gain, route_ids, route_weights,
    gate_weight, up_weight, down_weight, shared_gate, shared_up, shared_down,
):
    positions = (lax.axis_index("ep") * ROWS).astype(F32) + jnp.arange(ROWS, dtype=F32)
    inverse = 1.0 / ROPE_BASE ** (jnp.arange(ROPE // 2, dtype=F32) * 2.0 / ROPE)
    angles = inverse[:, None] * positions[None, :]
    return fused(
        (
            second_rows, second_gain.reshape(1, -1), route_ids.T, route_weights.T,
            query_latent, query_gain.reshape(1, -1), keyval_latent, keyval_gain.reshape(1, -1),
            rotary_key.T, jnp.cos(angles), jnp.sin(angles), output_gain.reshape(1, -1),
        ),
        (
            keyval_weight, shared_gate, shared_up, shared_down, query_weight,
            gate_weight[0], up_weight[0], down_weight[0], output_weight,
        ),
    )


def solution(mesh):
    placed = (
        P("ep", None), P("ep", None), P("ep", None), P(), P(), P(None, "tp"), P(None, "tp"),
        P("tp", None), P(), P("ep", None), P(), P("ep", None), P("ep", None),
        P("ep", None, "tp"), P("ep", None, "tp"), P("ep", "tp", None),
        P(None, "tp"), P(None, "tp"), P("tp", None),
    )
    return jax.shard_map(
        per_device,
        mesh=mesh,
        in_specs=placed,
        out_specs=(P(("ep", "tp"), None), P("ep", "tp")),
        check_vma=False,
    )
```
